32 devices in a mesh: sp: 16 (over z, y, core), tp: 2 (over x).
Axes of the slice: x: 2, y: 2, z: 4, core: 2. Of those that a mesh axis runs over, the one named last changes fastest.
Arguments:
- residual: bfloat16 [2048, 2048], P('sp', 'tp'), may hold values from -24 to 24
- queries: bfloat16 [2048, 2048], P('sp', 'tp'), may hold values from -16 to 16
- key_proj: bfloat16 [2048, 512], P(('sp', 'tp')), may hold values from -8 to 8
- value_proj: bfloat16 [2048, 512], P(('sp', 'tp')), may hold values from -6 to 6
- diff_lambda: float32 [8], replicated, may hold values from 0.3 to 0.8
- head_gain: float32 [256], replicated, may hold values from 0.1 to 1.9
- out_weight: bfloat16 [2048, 2048], P(None, 'tp'), may hold values from -0.125 to 0.125
- norm_gain: float32 [2048], P('tp'), may hold values from 0.1 to 1.9
- up_weight: bfloat16 [2048, 8192], P('sp', 'tp'), may hold values from -0.125 to 0.125
- down_weight: bfloat16 [8192, 2048], P('tp', 'sp'), may hold values from -0.0625 to 0.0625
Outputs:
- layer_out: bfloat16 [2048, 2048], P('sp', 'tp')
The draws below stay inside these ranges and needn't reach their ends.
All inputs are finite; a program needn't handle non-finite values.
Results may differ from the reference program's by a relative error of at most 0.012.
Values may be sent and summed in bfloat16 or wider, within the bound.
A program may use at most 128 MiB of HBM per device.

```python
import jax
import jax.numpy as jnp
from jax import lax

D = 2048
HEADS = 8
KV_HEADS = 2
HEAD_DIM = 128
VALUE_DIM = 256
FF = 8192
TOK_DEV = 128
SEQ = 2048


def draw_residual(key, part):
    base = jax.random.fold_in(key, 11)
    first, second, third = jax.random.split(base, 3)
    noise = jax.random.truncated_normal(first, -3.0, 3.0, (SEQ, D), jnp.float32)
    column = jnp.arange(D, dtype=jnp.float32) / D
    rough = jnp.exp(jax.random.uniform(second, (1, D), jnp.float32, jnp.log(0.8), jnp.log(1.25)))
    col_scale = jnp.exp(jnp.log(0.3) + jnp.log(10.0) * column)[None, :] * rough
    row_scale = jnp.exp(jax.random.uniform(third, (SEQ, 1), jnp.float32, jnp.log(0.5), jnp.log(1.6)))
    return (noise * col_scale * row_scale).astype(jnp.bfloat16)


def drawn_pair(key):
    base = jax.random.fold_in(key, 23)
    streams = jax.random.split(base, 2)
    query_vals = 1.3 * jax.random.truncated_normal(streams[0], -6.0, 6.0, (SEQ, HEADS * 2 * HEAD_DIM), jnp.float32)
    key_vals = 1.3 * jax.random.truncated_normal(streams[1], -6.0, 6.0, (SEQ, KV_HEADS * 2 * HEAD_DIM), jnp.float32)
    return (query_vals, key_vals)


def draw_queries(key, part):
    return drawn_pair(key)[0].astype(jnp.bfloat16)


def draw_key_proj(key, part):
    return drawn_pair(key)[1].astype(jnp.bfloat16)


def levels(own_key, extent, cuts, least, largest):
    def one(position, shards_of):
        heights = jax.random.uniform(jax.random.fold_in(jax.random.fold_in(own_key, 6), position), (shards_of,), jnp.float32, least / len(cuts), largest / len(cuts))
        return jnp.repeat(jnp.exp(heights), extent[position] // shards_of).reshape((-1,) + (1,) * (len(extent) - position - 1))

    loudness = one(*cuts[0])
    for cut in cuts[1:]:
        loudness = loudness * one(*cut)
    return loudness


def normal_values(own_key, shape, deviation, most, shards=(), held_as=jnp.bfloat16):
    values = jax.random.normal(own_key, shape, jnp.float32) * deviation
    if len(shards) > 0:
        values = levels(own_key, shape, shards, -0.22, 0.18) * values
    return jnp.clip(values, min=-most, max=most).astype(held_as)


def setup_inputs(seed: int = 0) -> dict:
    key_list = jax.random.split(jax.random.key(seed), 11)
    residual = draw_residual(jax.random.fold_in(key_list[10], 71), 0)
    queries = draw_queries(jax.random.fold_in(key_list[10], 71), 0)
    key_proj = draw_key_proj(jax.random.fold_in(key_list[10], 71), 0)
    value_proj = normal_values(key_list[3], (SEQ, KV_HEADS * VALUE_DIM), 1.0, 6.0, ((0, 32),))
    diff_lambda = jnp.clip(jax.random.uniform(key_list[4], (HEADS,), jnp.float32, 0.3, 0.8), 0.3, 0.8)
    head_gain = jnp.clip(1.0 + 0.18 * jax.random.normal(key_list[5], (VALUE_DIM,), jnp.float32), 0.1, 1.9)
    out_weight = normal_values(key_list[6], (HEADS * VALUE_DIM, D), (HEADS * VALUE_DIM) ** -0.5, 0.125, ((1, 2),))
    norm_gain = jnp.clip(1.0 + 0.18 * jax.random.normal(key_list[7], (D,), jnp.float32), 0.1, 1.9)
    up_weight = normal_values(key_list[8], (D, FF), D ** -0.5, 0.125, ((0, 16), (1, 2)))
    down_weight = normal_values(key_list[9], (FF, D), FF ** -0.5, 0.0625, ((0, 2), (1, 16)))
    return dict(residual=residual, queries=queries, key_proj=key_proj, value_proj=value_proj, diff_lambda=diff_lambda, head_gain=head_gain, out_weight=out_weight, norm_gain=norm_gain, up_weight=up_weight, down_weight=down_weight)


epsilon = 1e-06

def reference(residual, queries, key_proj, value_proj, diff_lambda, head_gain, out_weight, norm_gain, up_weight, down_weight):
    per_group = HEADS // KV_HEADS
    seq_len = queries.shape[0]
    scaling = HEAD_DIM ** (-0.5)
    key_grid = key_proj.astype(jnp.float32).reshape(seq_len, KV_HEADS, 2, HEAD_DIM)
    value_grid = value_proj.astype(jnp.float32).reshape(seq_len, KV_HEADS, VALUE_DIM)
    lambdas = diff_lambda.reshape(KV_HEADS, per_group, 1, 1)
    blocks = queries.reshape(seq_len // TOK_DEV, TOK_DEV, KV_HEADS, per_group, 2, HEAD_DIM)

    def one_block(query_block):
        query_float = query_block.astype(jnp.float32)
        scores = jnp.einsum('qagcd,kacd->agcqk', query_float, key_grid) * scaling
        highest = lax.optimization_barrier(jnp.max(scores, axis=-1, keepdims=True))
        weights = jnp.exp(scores - highest)
        totals = lax.optimization_barrier(jnp.sum(weights, axis=-1))
        rounded = lax.optimization_barrier(weights.astype(jnp.bfloat16)).astype(jnp.float32)
        summed = jnp.einsum('agcqk,kae->agcqe', rounded, value_grid)
        per_map = summed / totals[..., None]
        difference = per_map[:, :, 0] - lambdas * per_map[:, :, 1]
        normed = difference * lax.rsqrt(lax.optimization_barrier(jnp.mean(difference * difference, axis=-1, keepdims=True)) + epsilon) * head_gain
        return normed.astype(jnp.bfloat16).reshape(HEADS, TOK_DEV, VALUE_DIM)
    outputs = lax.map(one_block, blocks)
    head_outputs = outputs.transpose(1, 0, 2, 3).reshape(HEADS, seq_len, VALUE_DIM)
    out_grid = out_weight.reshape(HEADS, VALUE_DIM, D)
    projected = jnp.einsum('hse,hed->sd', head_outputs.astype(jnp.float32), out_grid.astype(jnp.float32))
    after_mix = residual.astype(jnp.float32) + projected
    normed = (after_mix * lax.rsqrt(lax.optimization_barrier(jnp.mean(after_mix * after_mix, axis=1, keepdims=True)) + epsilon) * norm_gain).astype(jnp.bfloat16)
    hidden = jnp.dot(normed, up_weight, preferred_element_type=jnp.float32)
    activated = jnp.square(jax.nn.relu(hidden)).astype(jnp.bfloat16)
    mixed = jnp.dot(activated, down_weight, preferred_element_type=jnp.float32)
    return (after_mix + mixed).astype(jnp.bfloat16)
```

```python
import functools
import math

import jax
import jax.numpy as jnp
from jax import lax
from jax.experimental import pallas as pl
from jax.experimental.pallas import tpu as pltpu
from jax.sharding import PartitionSpec as P

D = 2048
HEADS = 8
KV_HEADS = 2
HEAD_DIM = 128
VALUE_DIM = 256


epsilon = 1e-06


def head_norm(per_map, lambdas, gain):
    difference = per_map[:, 0] - lambdas[:, None, None] * per_map[:, 1]
    scaled = (
        difference
        * lax.rsqrt(jnp.mean(difference * difference, axis=-1, keepdims=True) + epsilon)
        * gain
    )
    return scaled.astype(jnp.bfloat16)


def on_device(
    residual,
    queries,
    key_proj,
    value_proj,
    diff_lambda,
    head_gain,
    out_weight,
    norm_gain,
    up_weight,
    down_weight,
):
    rows_here = residual.shape[0]
    per_group = HEADS // KV_HEADS
    scaling = HEAD_DIM ** (-0.5)
    all_queries = lax.all_gather(queries, "tp", axis=1, tiled=True)
    query_grid = all_queries.reshape(rows_here, KV_HEADS, per_group, 2, HEAD_DIM)
    stat_shape = (KV_HEADS, per_group, 2, rows_here)
    maxima = jnp.full(stat_shape, -1e30, jnp.float32)
    key_piece = lax.all_gather(key_proj, "sp", axis=0, tiled=True)
    value_piece = lax.all_gather(value_proj, "sp", axis=0, tiled=True)
    key_count = key_piece.shape[0]
    key_grid = key_piece.reshape(key_count, KV_HEADS, 2, HEAD_DIM)
    value_grid = value_piece.reshape(key_count, KV_HEADS, VALUE_DIM)
    scores = (
        jnp.einsum("qagcd,kacd->agcqk", query_grid, key_grid, preferred_element_type=jnp.float32)
        * scaling
    )
    highest = jnp.maximum(maxima, jnp.max(scores, axis=-1))
    weights = jnp.exp(scores - highest[..., None])
    totals = jnp.sum(weights, axis=-1)
    weighted = jnp.einsum(
        "agcqk,kae->agcqe",
        weights.astype(jnp.bfloat16),
        value_grid,
        preferred_element_type=jnp.float32,
    )
    maxima, totals, weighted = (highest, totals, weighted)
    maxima = maxima.reshape(HEADS, 2, rows_here)
    totals = totals.reshape(HEADS, 2, rows_here)
    weighted = weighted.reshape(HEADS, 2, rows_here, VALUE_DIM)
    tp_size = lax.axis_size("tp")
    local_heads = HEADS // tp_size
    got_max, got_tot, got_sum = (
        lax.all_to_all(maxima, "tp", split_axis=0, concat_axis=0, tiled=True),
        lax.all_to_all(totals, "tp", split_axis=0, concat_axis=0, tiled=True),
        lax.all_to_all(weighted, "tp", split_axis=0, concat_axis=0, tiled=True),
    )
    got_max = got_max.reshape(tp_size, local_heads, 2, rows_here)
    got_tot = got_tot.reshape(tp_size, local_heads, 2, rows_here)
    got_sum = got_sum.reshape(tp_size, local_heads, 2, rows_here, VALUE_DIM)
    highest = jnp.max(got_max, axis=0)
    factor = jnp.exp(got_max - highest)
    totals_all = jnp.sum(factor * got_tot, axis=0)
    sums_all = jnp.sum(factor[..., None] * got_sum, axis=0)
    lambdas = lax.dynamic_slice_in_dim(diff_lambda, lax.axis_index("tp") * local_heads, local_heads)
    own_heads = head_norm(sums_all / totals_all[..., None], lambdas, head_gain)
    head_outputs = lax.all_gather(own_heads, "tp", axis=0, tiled=True)
    out_grid = out_weight.reshape(HEADS, VALUE_DIM, out_weight.shape[1])
    projected = jnp.einsum(
        "hqe,hed->qd", head_outputs, out_grid, preferred_element_type=jnp.float32
    )
    after_mix = residual.astype(jnp.float32) + projected
    squares = lax.psum(jnp.sum(after_mix * after_mix, axis=1), "tp")
    normed = (after_mix * lax.rsqrt(squares / D + epsilon)[:, None] * norm_gain).astype(
        jnp.bfloat16
    )
    full_rows = lax.all_gather(normed, "tp", axis=1, tiled=True)
    hidden = jnp.dot(
        full_rows,
        lax.all_gather(up_weight, "sp", axis=0, tiled=True),
        preferred_element_type=jnp.float32,
    )
    activated = jnp.square(jax.nn.relu(hidden)).astype(jnp.bfloat16)
    partial_value = jnp.dot(
        activated,
        lax.all_gather(down_weight, "sp", axis=1, tiled=True),
        preferred_element_type=jnp.float32,
    )
    mixer_sum = lax.psum_scatter(partial_value, "tp", scatter_dimension=1, tiled=True)
    return (after_mix + mixer_sum).astype(jnp.bfloat16)


MESH = pl.DeviceIdType.MESH
F32 = jnp.float32
BF16 = jnp.bfloat16
CHIP_CORES = 2
Y_CHIPS = 2


def fused_kernel(
    layers, residual, queries, keys, values, lambdas, head_gain, out_weight, norm_gain,
    up, down, out,
    kv_all, up_all, down_all, q_buf, res_buf, w_buf, heads_all, squares, tokens,
    part_out, part_in, sum_out, sum_in, after, own_part, local_sem, send_sem, recv_sem,
):
    x = lax.axis_index("tp")
    s = lax.axis_index("sp")
    core, y, z = s % CHIP_CORES, (s // CHIP_CORES) % Y_CHIPS, s // (CHIP_CORES * Y_CHIPS)

    def place(z_, y_, c_):
        return (z_ * Y_CHIPS + y_) * CHIP_CORES + c_

    def z_back(d):
        return lax.rem(z - d + layers, layers)

    def z_ahead(d):
        return lax.rem(z + d, layers)

    mate = {"sp": s, "tp": 1 - x}
    beside = {"sp": place(z, 1 - y, core), "tp": x}
    twin = {"sp": place(z, y, 1 - core), "tp": x}
    column = [{"sp": place(z_ahead(d), y, core), "tp": x} for d in range(layers)]

    barrier = pltpu.get_barrier_semaphore()
    peers = [mate, beside, twin] + column[1:]
    for peer in peers:
        pl.semaphore_signal(barrier, inc=1, device_id=peer, device_id_type=MESH)

    count = {"local": 0, "remote": 0}
    started = []

    def bring(src, dst):
        copy = pltpu.make_async_copy(src, dst, local_sem.at[count["local"]])
        count["local"] += 1
        copy.start()
        return copy

    def send(src, dst, peer):
        i = count["remote"]
        count["remote"] += 1
        copy = pltpu.make_async_remote_copy(
            src_ref=src, dst_ref=dst, send_sem=send_sem.at[i], recv_sem=recv_sem.at[i],
            device_id=peer, device_id_type=MESH,
        )
        copy.start()
        started.append(copy)
        return copy

    few = keys.shape[0]
    kw = kv_all.shape[2] // 2
    chunk = up_all.shape[2]
    lanes = down.shape[1]

    def half(ref, part):
        return ref.at[:, pl.ds(pl.multiple_of(part * kw, kw), kw)]

    def kv_rows(block, part, side):
        return kv_all.at[block, pl.ds(pl.multiple_of(part * few, few), few), pl.ds(side * kw, kw)]

    own_kv = [bring(half(keys, x), kv_rows(s, x, 0)), bring(half(values, x), kv_rows(s, x, 1))]
    q_copy = bring(queries, q_buf)

    pl.semaphore_wait(barrier, len(peers))

    swapped = [
        send(half(keys, 1 - x), kv_rows(s, x, 0), mate),
        send(half(values, 1 - x), kv_rows(s, x, 1), mate),
    ]
    for copy in own_kv:
        copy.wait()
    for copy in swapped:
        copy.wait_recv()
    kv_z = [None] + [send(kv_all.at[s], kv_all.at[s], column[d]) for d in range(1, layers)]

    def up_chunk(part):
        return up.at[:, pl.ds(pl.multiple_of(part * chunk, chunk), chunk)]

    def down_chunk(part):
        return down.at[pl.ds(pl.multiple_of(part * chunk, chunk), chunk), :]

    def up_block(b):
        return up_all.at[b]

    def down_block(b):
        return down_all.at[:, pl.ds(pl.multiple_of(b * lanes, lanes), lanes)]

    up_z = [None] + [send(up_chunk(z_ahead(d)), up_block(s), column[d]) for d in range(1, layers)]
    up_own = bring(up_chunk(z), up_block(s))
    down_own = bring(down_chunk(z), down_block(s))
    w_copy = bring(out_weight, w_buf)
    r_copy = bring(residual, res_buf)

    def spread(block_of, d, arrival):
        if arrival is not None:
            arrival()
        b = block_of(place(z_back(d), y, core))
        return send(b, b, beside), send(b, b, twin)

    def pass_on(block_of, d, came):
        came.wait_recv()
        b = block_of(place(z_back(d), 1 - y, core))
        return send(b, b, twin)

    def kv_block(b):
        return kv_all.at[b]

    kv_y, kv_t, kv_u = [], [], []
    for d in range(layers):
        to_y, to_t = spread(kv_block, d, kv_z[d].wait_recv if d else None)
        kv_y.append(to_y)
        kv_t.append(to_t)
        if d:
            kv_u.append(pass_on(kv_block, d - 1, kv_y[d - 1]))
    kv_u.append(pass_on(kv_block, layers - 1, kv_y[layers - 1]))

    up_y, up_t, up_u = {}, {}, {}
    down_y, down_t, down_u = {}, {}, {}
    up_y[0], up_t[0] = spread(up_block, 0, up_own.wait)
    down_z = [None] + [
        send(down_chunk(z_ahead(d)), down_block(s), column[d]) for d in range(1, layers)
    ]
    for copy in kv_t + kv_u:
        copy.wait_recv()
    q_copy.wait()

    local_heads = q_buf.shape[1] // (2 * HEAD_DIM)
    blocks, per_block = kv_all.shape[0], kv_all.shape[1]
    key_count = blocks * per_block
    factor = HEAD_DIM ** (-0.5) * math.log2(math.e)
    vals = lambda: kv_all[:, :, kw:].reshape(key_count, kw)
    head_copies = []
    for h in range(local_heads):
        maps = []
        for c in range(2):
            q = q_buf[:, (2 * h + c) * HEAD_DIM : (2 * h + c + 1) * HEAD_DIM]
            k = kv_all[:, :, c * HEAD_DIM : (c + 1) * HEAD_DIM].reshape(key_count, HEAD_DIM)
            scores = lax.dot_general(q, k, (((1,), (1,)), ((), ())), preferred_element_type=F32)
            top = jnp.max(scores, axis=1, keepdims=True)
            weights = jnp.exp2((scores - top) * factor)
            total = jnp.sum(weights, axis=1, keepdims=True)
            summed = jnp.dot(weights.astype(BF16), vals(), preferred_element_type=F32)
            maps.append(summed / total)
        diff = maps[0] - lambdas[x * local_heads + h] * maps[1]
        scaled = diff * lax.rsqrt(jnp.mean(diff * diff, axis=1, keepdims=True) + epsilon)
        where = heads_all.at[x, :, pl.ds(h * VALUE_DIM, VALUE_DIM)]
        heads_all[x, :, pl.ds(h * VALUE_DIM, VALUE_DIM)] = (scaled * head_gain[...]).astype(BF16)
        head_copies.append(send(where, where, mate))
        if 1 <= h < layers:
            up_y[h], up_t[h] = spread(up_block, h, up_z[h].wait_recv)
            up_u[h - 1] = pass_on(up_block, h - 1, up_y[h - 1])
    for d in range(max(local_heads, 1), layers):
        up_y[d], up_t[d] = spread(up_block, d, up_z[d].wait_recv)
        up_u[d - 1] = pass_on(up_block, d - 1, up_y[d - 1])

    wide = heads_all.shape[2]
    w_copy.wait()
    r_copy.wait()

    def w_rows(part):
        return w_buf[pl.ds(pl.multiple_of(part * wide, wide), wide), :]

    mix = res_buf[...].astype(F32) + jnp.dot(heads_all[x], w_rows(x), preferred_element_type=F32)
    down_y[0], down_t[0] = spread(down_block, 0, down_own.wait)
    for copy in head_copies:
        copy.wait_recv()
    mix = mix + jnp.dot(heads_all[1 - x], w_rows(1 - x), preferred_element_type=F32)
    after[...] = mix
    own_squares = jnp.sum(mix * mix, axis=1, keepdims=True)
    squares[x] = jnp.broadcast_to(own_squares, squares.shape[1:])
    sq_copy = send(squares.at[x], squares.at[x], mate)
    up_u[layers - 1] = pass_on(up_block, layers - 1, up_y[layers - 1])
    sq_copy.wait_recv()
    width = 2 * wide
    mean = (own_squares + squares[1 - x][:, :1]) / width
    tokens[z, x] = (after[...] * lax.rsqrt(mean + epsilon) * norm_gain[...]).astype(BF16)

    mine = tokens.at[z, x]
    tok_z = [None] + [send(mine, mine, column[d]) for d in range(1, layers)]
    tok_x = [send(mine, mine, mate)]
    for d in range(1, layers):
        down_y[d], down_t[d] = spread(down_block, d, down_z[d].wait_recv)
        down_u[d - 1] = pass_on(down_block, d - 1, down_y[d - 1])
    down_u[layers - 1] = pass_on(down_block, layers - 1, down_y[layers - 1])
    for d in range(1, layers):
        tok_z[d].wait_recv()
        block = tokens.at[z_back(d), x]
        tok_x.append(send(block, block, mate))
    for group in (up_t, up_u, down_t, down_u):
        for d in range(layers):
            group[d].wait_recv()

    up_half = up_all.shape[0] // 2
    order = list(range(layers))
    part_copies, sum_copies = {}, {}

    def up_rows(i):
        return up_all[i * up_half : (i + 1) * up_half].reshape(wide, chunk)

    def settle(d):
        part_copies[d].wait_recv()
        both = own_part[d] + part_in[d].astype(F32)
        if d == 0:
            after[...] = after[...] + both
        else:
            sum_out[d - 1] = both.astype(BF16)
            back = {"sp": place(z_back(d), y, core), "tp": x}
            sum_copies[d] = send(sum_out.at[d - 1], sum_in.at[d - 1], back)

    for i, d in enumerate(order):
        zb = z_back(d)
        tok_x[d].wait_recv()
        hidden = jnp.dot(tokens[zb, 0], up_rows(0), preferred_element_type=F32) + jnp.dot(
            tokens[zb, 1], up_rows(1), preferred_element_type=F32
        )
        activated = jnp.square(jnp.maximum(hidden, 0.0)).astype(BF16)

        def down_cols(part):
            return down_all[:, pl.ds(pl.multiple_of(part * wide, wide), wide)]

        part_out[d] = jnp.dot(activated, down_cols(1 - x), preferred_element_type=F32).astype(BF16)
        part_copies[d] = send(part_out.at[d], part_in.at[d], mate)
        own_part[d] = jnp.dot(activated, down_cols(x), preferred_element_type=F32)
        if i:
            settle(order[i - 1])
    settle(order[-1])
    result = after[...]
    for d in range(1, layers):
        sum_copies[d].wait_recv()
        result = result + sum_in[d - 1].astype(F32)
    out[...] = result.astype(out.dtype)
    for copy in started:
        copy.wait_send()


def on_chip(sp_size, residual, queries, key_proj, value_proj, diff_lambda, head_gain, out_weight,
            norm_gain, up_weight, down_weight):
    layers = sp_size // (CHIP_CORES * Y_CHIPS)
    rows, wide = residual.shape
    kw = key_proj.shape[1] // KV_HEADS
    chunk = up_weight.shape[1] // layers
    hbm = pl.BlockSpec(memory_space=pltpu.HBM)
    vmem = pl.BlockSpec(memory_space=pltpu.VMEM)
    smem = pl.BlockSpec(memory_space=pltpu.SMEM)
    copies = 2 + 3 * (layers - 1) + 3 * 3 * layers + wide // VALUE_DIM + 1 + 3 * layers + layers
    return pl.pallas_call(
        functools.partial(fused_kernel, layers),
        out_shape=jax.ShapeDtypeStruct(residual.shape, BF16),
        in_specs=[hbm, hbm, hbm, hbm, smem, vmem, hbm, vmem, hbm, hbm],
        out_specs=vmem,
        scratch_shapes=[
            pltpu.VMEM((sp_size, 2 * key_proj.shape[0], 2 * kw), BF16),
            pltpu.VMEM((sp_size, up_weight.shape[0], chunk), BF16),
            pltpu.VMEM((chunk, sp_size * down_weight.shape[1]), BF16),
            pltpu.VMEM(queries.shape, BF16),
            pltpu.VMEM(residual.shape, BF16),
            pltpu.VMEM(out_weight.shape, BF16),
            pltpu.VMEM((2, rows, wide), BF16),
            pltpu.VMEM((2, rows, 128), F32),
            pltpu.VMEM((layers, 2, rows, wide), BF16),
            pltpu.VMEM((layers, rows, wide), BF16),
            pltpu.VMEM((layers, rows, wide), BF16),
            pltpu.VMEM((layers - 1, rows, wide), BF16),
            pltpu.VMEM((layers - 1, rows, wide), BF16),
            pltpu.VMEM((rows, wide), F32),
            pltpu.VMEM((layers, rows, wide), F32),
            pltpu.SemaphoreType.DMA((8,)),
            pltpu.SemaphoreType.DMA((copies,)),
            pltpu.SemaphoreType.DMA((copies,)),
        ],
        compiler_params=pltpu.CompilerParams(
            collective_id=0, has_side_effects=True, vmem_limit_bytes=60 * 2**20
        ),
        name="fused_layer",
    )(residual, queries, key_proj, value_proj, diff_lambda, head_gain.reshape(1, -1), out_weight,
      norm_gain.reshape(1, -1), up_weight, down_weight)


def solution(mesh):
    sp_size, tp_size = mesh.shape["sp"], mesh.shape["tp"]
    direct = tp_size == KV_HEADS == 2 and sp_size % (CHIP_CORES * Y_CHIPS) == 0
    body = functools.partial(on_chip, sp_size) if direct else on_device
    return jax.shard_map(
        body,
        mesh=mesh,
        in_specs=(
            P("sp", "tp"),
            P("sp", "tp"),
            P(("sp", "tp"), None),
            P(("sp", "tp"), None),
            P(),
            P(),
            P(None, "tp"),
            P("tp"),
            P("sp", "tp"),
            P("tp", "sp"),
        ),
        out_specs=P("sp", "tp"),
        check_vma=False,
    )
```

```python
import functools
import math

import jax
import jax.numpy as jnp
from jax import lax
from jax.experimental import pallas as pl
from jax.experimental.pallas import tpu as pltpu
from jax.sharding import PartitionSpec as P

D = 2048
HEADS = 8
KV_HEADS = 2
HEAD_DIM = 128
VALUE_DIM = 256


epsilon = 1e-06


def head_norm(per_map, lambdas, gain):
    difference = per_map[:, 0] - lambdas[:, None, None] * per_map[:, 1]
    scaled = (
        difference
        * lax.rsqrt(jnp.mean(difference * difference, axis=-1, keepdims=True) + epsilon)
        * gain
    )
    return scaled.astype(jnp.bfloat16)


def on_device(
    residual,
    queries,
    key_proj,
    value_proj,
    diff_lambda,
    head_gain,
    out_weight,
    norm_gain,
    up_weight,
    down_weight,
):
    rows_here = residual.shape[0]
    per_group = HEADS // KV_HEADS
    scaling = HEAD_DIM ** (-0.5)
    all_queries = lax.all_gather(queries, "tp", axis=1, tiled=True)
    query_grid = all_queries.reshape(rows_here, KV_HEADS, per_group, 2, HEAD_DIM)
    stat_shape = (KV_HEADS, per_group, 2, rows_here)
    maxima = jnp.full(stat_shape, -1e30, jnp.float32)
    key_piece = lax.all_gather(key_proj, "sp", axis=0, tiled=True)
    value_piece = lax.all_gather(value_proj, "sp", axis=0, tiled=True)
    key_count = key_piece.shape[0]
    key_grid = key_piece.reshape(key_count, KV_HEADS, 2, HEAD_DIM)
    value_grid = value_piece.reshape(key_count, KV_HEADS, VALUE_DIM)
    scores = (
        jnp.einsum("qagcd,kacd->agcqk", query_grid, key_grid, preferred_element_type=jnp.float32)
        * scaling
    )
    highest = jnp.maximum(maxima, jnp.max(scores, axis=-1))
    weights = jnp.exp(scores - highest[..., None])
    totals = jnp.sum(weights, axis=-1)
    weighted = jnp.einsum(
        "agcqk,kae->agcqe",
        weights.astype(jnp.bfloat16),
        value_grid,
        preferred_element_type=jnp.float32,
    )
    maxima, totals, weighted = (highest, totals, weighted)
    maxima = maxima.reshape(HEADS, 2, rows_here)
    totals = totals.reshape(HEADS, 2, rows_here)
    weighted = weighted.reshape(HEADS, 2, rows_here, VALUE_DIM)
    tp_size = lax.axis_size("tp")
    local_heads = HEADS // tp_size
    got_max, got_tot, got_sum = (
        lax.all_to_all(maxima, "tp", split_axis=0, concat_axis=0, tiled=True),
        lax.all_to_all(totals, "tp", split_axis=0, concat_axis=0, tiled=True),
        lax.all_to_all(weighted, "tp", split_axis=0, concat_axis=0, tiled=True),
    )
    got_max = got_max.reshape(tp_size, local_heads, 2, rows_here)
    got_tot = got_tot.reshape(tp_size, local_heads, 2, rows_here)
    got_sum = got_sum.reshape(tp_size, local_heads, 2, rows_here, VALUE_DIM)
    highest = jnp.max(got_max, axis=0)
    factor = jnp.exp(got_max - highest)
    totals_all = jnp.sum(factor * got_tot, axis=0)
    sums_all = jnp.sum(factor[..., None] * got_sum, axis=0)
    lambdas = lax.dynamic_slice_in_dim(diff_lambda, lax.axis_index("tp") * local_heads, local_heads)
    own_heads = head_norm(sums_all / totals_all[..., None], lambdas, head_gain)
    head_outputs = lax.all_gather(own_heads, "tp", axis=0, tiled=True)
    out_grid = out_weight.reshape(HEADS, VALUE_DIM, out_weight.shape[1])
    projected = jnp.einsum(
        "hqe,hed->qd", head_outputs, out_grid, preferred_element_type=jnp.float32
    )
    after_mix = residual.astype(jnp.float32) + projected
    squares = lax.psum(jnp.sum(after_mix * after_mix, axis=1), "tp")
    normed = (after_mix * lax.rsqrt(squares / D + epsilon)[:, None] * norm_gain).astype(
        jnp.bfloat16
    )
    full_rows = lax.all_gather(normed, "tp", axis=1, tiled=True)
    hidden = jnp.dot(
        full_rows,
        lax.all_gather(up_weight, "sp", axis=0, tiled=True),
        preferred_element_type=jnp.float32,
    )
    activated = jnp.square(jax.nn.relu(hidden)).astype(jnp.bfloat16)
    partial_value = jnp.dot(
        activated,
        lax.all_gather(down_weight, "sp", axis=1, tiled=True),
        preferred_element_type=jnp.float32,
    )
    mixer_sum = lax.psum_scatter(partial_value, "tp", scatter_dimension=1, tiled=True)
    return (after_mix + mixer_sum).astype(jnp.bfloat16)


MESH = pl.DeviceIdType.MESH
F32 = jnp.float32
BF16 = jnp.bfloat16
CHIP_CORES = 2
Y_CHIPS = 2


def fused_kernel(
    layers, residual, queries, keys, values, lambdas, head_gain, out_weight, norm_gain,
    up, down, out,
    kv_all, up_all, down_all, q_buf, res_buf, w_buf, heads_all, squares, tokens,
    part_out, part_in, sum_out, sum_in, after, own_part, local_sem, send_sem, recv_sem,
):
    x = lax.axis_index("tp")
    s = lax.axis_index("sp")
    core, y, z = s % CHIP_CORES, (s // CHIP_CORES) % Y_CHIPS, s // (CHIP_CORES * Y_CHIPS)

    def place(z_, y_, c_):
        return (z_ * Y_CHIPS + y_) * CHIP_CORES + c_

    def z_back(d):
        return lax.rem(z - d + layers, layers)

    def z_ahead(d):
        return lax.rem(z + d, layers)

    mate = {"sp": s, "tp": 1 - x}
    beside = {"sp": place(z, 1 - y, core), "tp": x}
    twin = {"sp": place(z, y, 1 - core), "tp": x}
    column = [{"sp": place(z_ahead(d), y, core), "tp": x} for d in range(layers)]

    barrier = pltpu.get_barrier_semaphore()
    peers = [mate, beside, twin] + column[1:]
    for peer in peers:
        pl.semaphore_signal(barrier, inc=1, device_id=peer, device_id_type=MESH)

    count = {"local": 0, "remote": 0}
    started = []

    def bring(src, dst):
        copy = pltpu.make_async_copy(src, dst, local_sem.at[count["local"]])
        count["local"] += 1
        copy.start()
        return copy

    def send(src, dst, peer):
        i = count["remote"]
        count["remote"] += 1
        copy = pltpu.make_async_remote_copy(
            src_ref=src, dst_ref=dst, send_sem=send_sem.at[i], recv_sem=recv_sem.at[i],
            device_id=peer, device_id_type=MESH,
        )
        copy.start()
        started.append(copy)
        return copy

    few = keys.shape[0]
    kw = kv_all.shape[2] // 2
    chunk = up_all.shape[2]
    lanes = down.shape[1]

    def half(ref, part):
        return ref.at[:, pl.ds(pl.multiple_of(part * kw, kw), kw)]

    def kv_rows(block, part, side):
        return kv_all.at[block, pl.ds(pl.multiple_of(part * few, few), few), pl.ds(side * kw, kw)]

    own_kv = [bring(half(keys, x), kv_rows(s, x, 0)), bring(half(values, x), kv_rows(s, x, 1))]
    q_copy = bring(queries, q_buf)

    pl.semaphore_wait(barrier, len(peers))

    swapped = [
        send(half(keys, 1 - x), kv_rows(s, x, 0), mate),
        send(half(values, 1 - x), kv_rows(s, x, 1), mate),
    ]
    for copy in own_kv:
        copy.wait()
    for copy in swapped:
        copy.wait_recv()
    kv_z = [None] + [send(kv_all.at[s], kv_all.at[s], column[d]) for d in range(1, layers)]

    def up_chunk(part):
        return up.at[:, pl.ds(pl.multiple_of(part * chunk, chunk), chunk)]

    def down_chunk(part):
        return down.at[pl.ds(pl.multiple_of(part * chunk, chunk), chunk), :]

    def up_block(b):
        return up_all.at[b]

    def down_block(b):
        return down_all.at[:, pl.ds(pl.multiple_of(b * lanes, lanes), lanes)]

    up_z = [None] + [send(up_chunk(z_ahead(d)), up_block(s), column[d]) for d in range(1, layers)]
    up_own = bring(up_chunk(z), up_block(s))
    down_own = bring(down_chunk(z), down_block(s))
    w_copy = bring(out_weight, w_buf)
    r_copy = bring(residual, res_buf)

    def spread(block_of, d, arrival):
        if arrival is not None:
            arrival()
        b = block_of(place(z_back(d), y, core))
        return send(b, b, beside), send(b, b, twin)

    def pass_on(block_of, d, came):
        came.wait_recv()
        b = block_of(place(z_back(d), 1 - y, core))
        return send(b, b, twin)

    def kv_block(b):
        return kv_all.at[b]

    up_y, up_t, up_u = {}, {}, {}
    down_y, down_t, down_u = {}, {}, {}
    kv_y, kv_t, kv_u = [], [], []
    for d in range(layers):
        to_y, to_t = spread(kv_block, d, kv_z[d].wait_recv if d else None)
        kv_y.append(to_y)
        kv_t.append(to_t)
        if d:
            kv_u.append(pass_on(kv_block, d - 1, kv_y[d - 1]))
        else:
            up_y[0], up_t[0] = spread(up_block, 0, up_own.wait)
            down_z = [None] + [
                send(down_chunk(z_ahead(e)), down_block(s), column[e]) for e in range(1, layers)
            ]
    kv_u.append(pass_on(kv_block, layers - 1, kv_y[layers - 1]))

    down_y[0], down_t[0] = spread(down_block, 0, down_own.wait)
    for copy in kv_t + kv_u:
        copy.wait_recv()
    q_copy.wait()

    local_heads = q_buf.shape[1] // (2 * HEAD_DIM)
    blocks, per_block = kv_all.shape[0], kv_all.shape[1]
    key_count = blocks * per_block
    factor = HEAD_DIM ** (-0.5) * math.log2(math.e)
    vals = lambda: kv_all[:, :, kw:].reshape(key_count, kw)
    head_copies = []
    for h in range(local_heads):
        maps = []
        for c in range(2):
            q = q_buf[:, (2 * h + c) * HEAD_DIM : (2 * h + c + 1) * HEAD_DIM]
            k = kv_all[:, :, c * HEAD_DIM : (c + 1) * HEAD_DIM].reshape(key_count, HEAD_DIM)
            scores = lax.dot_general(q, k, (((1,), (1,)), ((), ())), preferred_element_type=F32)
            top = jnp.max(scores, axis=1, keepdims=True)
            weights = jnp.exp2((scores - top) * factor)
            total = jnp.sum(weights, axis=1, keepdims=True)
            summed = jnp.dot(weights.astype(BF16), vals(), preferred_element_type=F32)
            maps.append(summed / total)
        diff = maps[0] - lambdas[x * local_heads + h] * maps[1]
        scaled = diff * lax.rsqrt(jnp.mean(diff * diff, axis=1, keepdims=True) + epsilon)
        where = heads_all.at[x, :, pl.ds(h * VALUE_DIM, VALUE_DIM)]
        heads_all[x, :, pl.ds(h * VALUE_DIM, VALUE_DIM)] = (scaled * head_gain[...]).astype(BF16)
        head_copies.append(send(where, where, mate))
        if 1 <= h < layers:
            up_y[h], up_t[h] = spread(up_block, h, up_z[h].wait_recv)
    for d in range(max(local_heads, 1), layers):
        up_y[d], up_t[d] = spread(up_block, d, up_z[d].wait_recv)

    wide = heads_all.shape[2]
    w_copy.wait()
    r_copy.wait()

    def w_rows(part):
        return w_buf[pl.ds(pl.multiple_of(part * wide, wide), wide), :]

    mix = res_buf[...].astype(F32) + jnp.dot(heads_all[x], w_rows(x), preferred_element_type=F32)
    for copy in head_copies:
        copy.wait_recv()
    mix = mix + jnp.dot(heads_all[1 - x], w_rows(1 - x), preferred_element_type=F32)
    after[...] = mix
    own_squares = jnp.sum(mix * mix, axis=1, keepdims=True)
    squares[x] = jnp.broadcast_to(own_squares, squares.shape[1:])
    sq_copy = send(squares.at[x], squares.at[x], mate)
    sq_copy.wait_recv()
    width = 2 * wide
    mean = (own_squares + squares[1 - x][:, :1]) / width
    tokens[z, x] = (after[...] * lax.rsqrt(mean + epsilon) * norm_gain[...]).astype(BF16)

    mine = tokens.at[z, x]
    tok_z = [None] + [send(mine, mine, column[d]) for d in range(1, layers)]
    tok_x = {0: send(mine, mine, mate)}
    for d in range(1, layers):
        up_u[d - 1] = pass_on(up_block, d - 1, up_y[d - 1])
        down_y[d], down_t[d] = spread(down_block, d, down_z[d].wait_recv)
    up_u[layers - 1] = pass_on(up_block, layers - 1, up_y[layers - 1])
    down_u[0] = pass_on(down_block, 0, down_y[0])

    def cross(d):
        tok_z[d].wait_recv()
        block = tokens.at[z_back(d), x]
        tok_x[d] = send(block, block, mate)

    order = list(range(1, layers)) + [0]
    for d in order[:1]:
        cross(d)
    for d in range(1, layers):
        down_u[d] = pass_on(down_block, d, down_y[d])
    for d in order[1:-1][:1]:
        cross(d)
    for group in (up_t, up_u, down_t, down_u):
        for d in range(layers):
            group[d].wait_recv()

    up_half = up_all.shape[0] // 2
    part_copies, sum_copies = {}, {}

    def up_rows(i):
        return up_all[i * up_half : (i + 1) * up_half].reshape(wide, chunk)

    def settle(d):
        part_copies[d].wait_recv()
        both = own_part[d] + part_in[d].astype(F32)
        if d == 0:
            after[...] = after[...] + both
        else:
            sum_out[d - 1] = both.astype(BF16)
            back = {"sp": place(z_back(d), y, core), "tp": x}
            sum_copies[d] = send(sum_out.at[d - 1], sum_in.at[d - 1], back)

    for i, d in enumerate(order):
        zb = z_back(d)
        tok_x[d].wait_recv()
        hidden = jnp.dot(tokens[zb, 0], up_rows(0), preferred_element_type=F32) + jnp.dot(
            tokens[zb, 1], up_rows(1), preferred_element_type=F32
        )
        activated = jnp.square(jnp.maximum(hidden, 0.0)).astype(BF16)

        def down_cols(part):
            return down_all[:, pl.ds(pl.multiple_of(part * wide, wide), wide)]

        part_out[d] = jnp.dot(activated, down_cols(1 - x), preferred_element_type=F32).astype(BF16)
        part_copies[d] = send(part_out.at[d], part_in.at[d], mate)
        own_part[d] = jnp.dot(activated, down_cols(x), preferred_element_type=F32)
        if i + 2 < layers - 1:
            cross(order[i + 2])
        if i:
            settle(order[i - 1])
    settle(order[-1])
    result = after[...]
    for d in range(1, layers):
        sum_copies[d].wait_recv()
        result = result + sum_in[d - 1].astype(F32)
    out[...] = result.astype(out.dtype)
    for copy in started:
        copy.wait_send()


def on_chip(sp_size, residual, queries, key_proj, value_proj, diff_lambda, head_gain, out_weight,
            norm_gain, up_weight, down_weight):
    layers = sp_size // (CHIP_CORES * Y_CHIPS)
    rows, wide = residual.shape
    kw = key_proj.shape[1] // KV_HEADS
    chunk = up_weight.shape[1] // layers
    hbm = pl.BlockSpec(memory_space=pltpu.HBM)
    vmem = pl.BlockSpec(memory_space=pltpu.VMEM)
    smem = pl.BlockSpec(memory_space=pltpu.SMEM)
    copies = 2 + 3 * (layers - 1) + 3 * 3 * layers + wide // VALUE_DIM + 1 + 3 * layers + layers
    return pl.pallas_call(
        functools.partial(fused_kernel, layers),
        out_shape=jax.ShapeDtypeStruct(residual.shape, BF16),
        in_specs=[hbm, hbm, hbm, hbm, smem, vmem, hbm, vmem, hbm, hbm],
        out_specs=vmem,
        scratch_shapes=[
            pltpu.VMEM((sp_size, 2 * key_proj.shape[0], 2 * kw), BF16),
            pltpu.VMEM((sp_size, up_weight.shape[0], chunk), BF16),
            pltpu.VMEM((chunk, sp_size * down_weight.shape[1]), BF16),
            pltpu.VMEM(queries.shape, BF16),
            pltpu.VMEM(residual.shape, BF16),
            pltpu.VMEM(out_weight.shape, BF16),
            pltpu.VMEM((2, rows, wide), BF16),
            pltpu.VMEM((2, rows, 128), F32),
            pltpu.VMEM((layers, 2, rows, wide), BF16),
            pltpu.VMEM((layers, rows, wide), BF16),
            pltpu.VMEM((layers, rows, wide), BF16),
            pltpu.VMEM((layers - 1, rows, wide), BF16),
            pltpu.VMEM((layers - 1, rows, wide), BF16),
            pltpu.VMEM((rows, wide), F32),
            pltpu.VMEM((layers, rows, wide), F32),
            pltpu.SemaphoreType.DMA((8,)),
            pltpu.SemaphoreType.DMA((copies,)),
            pltpu.SemaphoreType.DMA((copies,)),
        ],
        compiler_params=pltpu.CompilerParams(
            collective_id=0, has_side_effects=True, vmem_limit_bytes=60 * 2**20
        ),
        name="fused_layer",
    )(residual, queries, key_proj, value_proj, diff_lambda, head_gain.reshape(1, -1), out_weight,
      norm_gain.reshape(1, -1), up_weight, down_weight)


def solution(mesh):
    sp_size, tp_size = mesh.shape["sp"], mesh.shape["tp"]
    direct = tp_size == KV_HEADS == 2 and sp_size % (CHIP_CORES * Y_CHIPS) == 0
    body = functools.partial(on_chip, sp_size) if direct else on_device
    return jax.shard_map(
        body,
        mesh=mesh,
        in_specs=(
            P("sp", "tp"),
            P("sp", "tp"),
            P(("sp", "tp"), None),
            P(("sp", "tp"), None),
            P(),
            P(),
            P(None, "tp"),
            P("tp"),
            P("sp", "tp"),
            P("tp", "sp"),
        ),
        out_specs=P("sp", "tp"),
        check_vma=False,
    )
```
